512 devices in a mesh: ep: 32 (over z, core), tp: 16 (over y, x).
Axes of the slice: x: 4, y: 4, z: 16, core: 2. Of those that a mesh axis runs over, the one named last changes fastest.
Arguments:
- tokens: bfloat16 [4096, 2048], P('ep'), may hold values from -6 to 6
- selected: int32 [32, 1024], P(None, 'ep'), may hold values from -1 to 127, as said below
- affinity: float32 [32, 1024], P(None, 'ep'), may hold values from 0.05 to 1
- w_gate: bfloat16 [32, 2048, 2048], P('ep', None, 'tp'), may hold values from -0.125 to 0.125
- w_up: bfloat16 [32, 2048, 2048], P('ep', None, 'tp'), may hold values from -0.125 to 0.125
- w_down: bfloat16 [32, 2048, 2048], P('ep', 'tp'), may hold values from -0.125 to 0.125
Outputs:
- combined: bfloat16 [4096, 2048], P('ep', 'tp')
The draws below stay inside these ranges and needn't reach their ends.
Inputs may be any that keep to these rules, and one draw needn't show every extreme that they name: `selected`: row e holds 32 aligned groups of 32 entries; the live entries of group j are distinct positions within the j-th block of 128 tokens, stand at the front of the group and are followed by -1; each row has 512 live entries in all, the number in a group varies, and some group of every row is full.
All inputs are finite; a program needn't handle non-finite values.
Results may differ from the reference program's by a relative error of at most 0.015.
Values may be sent and summed in bfloat16 or wider, within the bound.
A program may use at most 64 MiB of HBM per device.

```python
import math
import jax
import jax.numpy as jnp
from jax import lax

D = 2048
FF = 2048
TOK_DEV = 128
EXPERTS = 32
TOKENS = 4096
PICK = 16
MOST = 32
SLOTS = 1024
N_EP = 32
N_TP = 16


def draw_selected(key, part):
    half = N_EP // 2
    block_scores = jax.random.randint(jax.random.fold_in(key, 11), (EXPERTS, N_EP), 0, 2 ** 20)
    block_order = jnp.argsort(block_scores * N_EP + jnp.arange(N_EP, dtype=jnp.int32)[None, :], axis=1, stable=True).astype(jnp.int32)
    inverse = jnp.argsort(block_order, axis=1, stable=True).astype(jnp.int32)
    shifts = jax.random.randint(jax.random.fold_in(key, 12), (EXPERTS, half), -PICK, PICK + 1)
    forced = jax.random.randint(jax.random.fold_in(key, 13), (EXPERTS,), 0, half)
    shifts = jnp.where(jnp.arange(half, dtype=jnp.int32)[None, :] == forced[:, None], PICK, shifts)
    counts_paired = jnp.concatenate([PICK + shifts, PICK - shifts], axis=1)
    counts = jnp.take_along_axis(counts_paired, inverse, axis=1)
    scores = jax.random.randint(jax.random.fold_in(key, 17), (EXPERTS, N_EP, TOK_DEV), 0, 2 ** 20)
    distinct = scores * TOK_DEV + jnp.arange(TOK_DEV, dtype=jnp.int32)[None, None, :]
    order = jnp.argsort(distinct, axis=2, stable=True).astype(jnp.int32)[:, :, :MOST]
    live = jnp.arange(MOST, dtype=jnp.int32)[None, None, :] < counts[:, :, None]
    picked = jnp.where(live, order, -1)
    return picked.reshape(EXPERTS, N_EP * MOST).astype(jnp.int32)


def shard_levels(rng, dims, shards, low, largest):
    loudness = 1.0
    for axis_at, shards_of in shards:
        steps = jax.random.uniform(jax.random.fold_in(jax.random.fold_in(rng, 6), axis_at), (shards_of,), jnp.float32, low / len(shards), largest / len(shards))
        loudness = loudness * jnp.repeat(jnp.exp(steps), dims[axis_at] // shards_of).reshape((-1,) + (1,) * (len(dims) - 1 - axis_at))
    return loudness


def normal_values(stream_key, dims, width, most, pieces=(), kind=jnp.bfloat16):
    values = jax.random.normal(stream_key, dims, jnp.float32) * width
    if len(pieces) > 0:
        values = shard_levels(stream_key, dims, pieces, -0.22, 0.18) * values
    return jnp.clip(values, min=-most, max=most).astype(kind)


def setup_inputs(seed: int = 0) -> dict:
    streams_of = jax.random.split(jax.random.key(seed), 7)
    tokens = normal_values(streams_of[0], (TOKENS, D), 1.0, 6.0, ((0, 32),))
    selected = draw_selected(jax.random.fold_in(streams_of[6], 71), 0)
    affinity = jnp.clip(jnp.exp(math.log(1.0) - 2.9957323 * jax.random.uniform(streams_of[2], (EXPERTS, SLOTS), jnp.float32) ** shard_levels(streams_of[2], (EXPERTS, SLOTS), ((1, 32),), -0.2, 0.2)), 0.05, 1.0)
    w_gate = normal_values(streams_of[3], (EXPERTS, D, FF), D ** -0.5, 0.125, ((0, 32), (2, 16)))
    w_up = normal_values(streams_of[4], (EXPERTS, D, FF), D ** -0.5, 0.125, ((0, 32), (2, 16)))
    w_down = normal_values(streams_of[5], (EXPERTS, FF, D), FF ** -0.5, 0.125, ((0, 32), (1, 16)))
    return {"tokens": tokens, "selected": selected, "affinity": affinity, "w_gate": w_gate, "w_up": w_up, "w_down": w_down}


def reference(tokens, selected, affinity, w_gate, w_up, w_down):
    offsets = (jnp.arange(SLOTS, dtype=jnp.int32) // MOST) * TOK_DEV

    def expert_step(carry, inputs):
        index_row, weight_row, gate_mat, up_mat, down_mat = inputs
        live = index_row >= 0
        position = (jnp.maximum(index_row, 0) + offsets).astype(jnp.int32)
        chosen = tokens[position]
        gate_act = jnp.dot(chosen, gate_mat, preferred_element_type=jnp.float32)
        up_act = jnp.dot(chosen, up_mat, preferred_element_type=jnp.float32)
        hidden = (jax.nn.silu(gate_act) * up_act).astype(jnp.bfloat16)
        blocks = hidden.reshape(SLOTS, N_TP, FF // N_TP).astype(jnp.float32)
        down_blocks = down_mat.reshape(N_TP, FF // N_TP, D).astype(jnp.float32)
        partial_value = jnp.einsum('ckf,kfd->kcd', blocks, down_blocks).astype(jnp.bfloat16)
        expert_out = jnp.sum(partial_value.astype(jnp.float32), axis=0).astype(jnp.bfloat16)
        scaled_weight = jnp.where(live, weight_row, jnp.zeros_like(weight_row))
        carry = carry.at[position].add(scaled_weight[:, None] * expert_out.astype(jnp.float32))
        return carry, None

    initial = jnp.zeros((TOKENS, D), jnp.float32)
    result, unused = lax.scan(expert_step, initial, (selected, affinity, w_gate, w_up, w_down))
    return result.astype(jnp.bfloat16)
```

```python
import functools

import jax
import jax.numpy as jnp
from jax import lax
from jax.experimental import pallas as pl
from jax.experimental.pallas import tpu as pltpu
from jax.sharding import PartitionSpec as P

MESH = pl.DeviceIdType.MESH
BF = jnp.bfloat16
F32 = jnp.float32

N_EP, N_TP, N_Z, SIDE = 32, 16, 16, 4
MOST, TOK, WID = 32, 128, 128
ROWS, CHUNK = 512, 128
CHUNKS = ROWS // CHUNK
HALF = CHUNK // 2
PER = CHUNK // MOST
EARLY = N_EP - PER * (CHUNKS - 1)
DEAD = 1024.0

PLACES = [(0, 0), (0, 1)]
for _d in range(1, N_Z // 2):
    PLACES += [(_d, 0), (_d, 1), (N_Z - _d, 0), (N_Z - _d, 1)]
PLACES += [(N_Z // 2, 0), (N_Z // 2, 1)]
SUM_ORDER = (0, 3, 2, 1)


def remote(src, dst, send, recv, device):
    return pltpu.make_async_remote_copy(
        src_ref=src, dst_ref=dst, send_sem=send, recv_sem=recv, device_id=device, device_id_type=MESH
    )


def kernel(
    tok, sel, aff, wg, wu, wd, out,
    tokb, selb, affb, wgu, wdb, onehot, sent, came, pick, spread, rows, part, got1, sum1, got2,
    result, back, home, mix,
    in_sem, z_send, z_recv, a1_send, a1_recv, a2_send, a2_recv,
    r1_send, r1_recv, r2_send, r2_recv, b_send, b_recv,
):
    ep, tp = lax.axis_index("ep"), lax.axis_index("tp")
    z, core = ep // 2, ep % 2
    y, x = tp // SIDE, tp % SIDE

    def ep_peer(i):
        dz, dc = PLACES[i]
        e = lax.rem(z + dz, N_Z) * 2 + lax.rem(core + dc, 2)
        return e, {"ep": e, "tp": tp}

    def ep_back(i):
        dz, dc = PLACES[i]
        e = lax.rem(z + N_Z - dz, N_Z) * 2 + lax.rem(core + dc, 2)
        return e, {"ep": e, "tp": tp}

    def line(axis, i):
        if axis == 0:
            t = y * SIDE + lax.rem(x + i, SIDE)
        else:
            t = lax.rem(y + i, SIDE) * SIDE + x
        return t, {"ep": ep, "tp": t}

    loads = [
        pltpu.make_async_copy(sel, selb, in_sem.at[0]),
        pltpu.make_async_copy(aff, affb, in_sem.at[1]),
        pltpu.make_async_copy(
            tok.at[:, pl.ds(pl.multiple_of(tp * WID, WID), WID)], tokb.at[pl.ds(0, TOK)], in_sem.at[2]
        ),
        pltpu.make_async_copy(wg, wgu.at[:, pl.ds(0, WID)], in_sem.at[3]),
        pltpu.make_async_copy(wu, wgu.at[:, pl.ds(WID, WID)], in_sem.at[4]),
        pltpu.make_async_copy(wd, wdb, in_sem.at[5]),
    ]
    for load in loads:
        load.start()
    barrier = pltpu.get_barrier_semaphore()
    peers = [ep_peer(i)[1] for i in range(1, N_EP)]
    peers += [line(a, i)[1] for a in (0, 1) for i in (1, 2, 3)]
    for peer in peers:
        pl.semaphore_signal(barrier, inc=1, device_id=peer, device_id_type=MESH)

    tokb[TOK : 2 * TOK] = jnp.full((TOK, WID), DEAD, BF)
    loads[0].wait()
    loads[1].wait()
    sel_t = selb[...].astype(F32).T
    aff_t = affb[...].T
    lane2 = lax.broadcasted_iota(jnp.int32, (MOST, 2 * TOK), 1).astype(F32)
    lane1 = lax.broadcasted_iota(jnp.int32, (MOST, TOK), 1).astype(F32)
    for e in range(N_EP):
        column = sel_t[:, e : e + 1]
        spot = jnp.where(column < 0.0, float(TOK), column)
        onehot[e * MOST : (e + 1) * MOST] = jnp.where(lane2 == spot, 1.0, 0.0).astype(BF)
    loads[2].wait()
    sent[...] = (
        jnp.dot(onehot[...], tokb[...], preferred_element_type=F32).astype(BF).reshape(N_EP, MOST, WID)
    )
    came[0] = sent[ep]
    pl.semaphore_wait(barrier, len(peers))

    zs = []
    for i in range(1, N_EP):
        e, peer = ep_peer(i)
        copy = remote(sent.at[e], came.at[i], z_send.at[i], z_recv.at[i], peer)
        copy.start()
        zs.append(copy)

    for q in range(N_EP * MOST // TOK):
        tall = []
        for e in range(q * PER, (q + 1) * PER):
            tall.append(jnp.where(lane1 == sel_t[:, e : e + 1], aff_t[:, e : e + 1], 0.0))
        wide = jnp.concatenate(tall, axis=0).T
        high = wide.astype(BF)
        mix[0, :, q * TOK : (q + 1) * TOK] = high
        mix[1, :, q * TOK : (q + 1) * TOK] = (wide - high.astype(F32)).astype(BF)

    lane_row = lax.broadcasted_iota(jnp.int32, (1, WID), 1)
    lane_slot = lax.rem(lane_row, MOST).astype(F32)
    lane_group = lane_row // MOST
    down_rows = lax.broadcasted_iota(jnp.int32, (CHUNK, WID), 0).astype(F32)

    starts, counts = [], []
    total = jnp.zeros((1, WID), F32)
    copies = {"a1": {}, "a2": {}, "r1": {}, "r2": {}}

    def span(c, half):
        return pl.ds(c * CHUNK + half * HALF, HALF)

    def begin_gather(c):
        for i in (2, 1, 3):
            for half in (0, 1):
                block = rows.at[tp, span(c, half)]
                copy = remote(
                    block, block, a1_send.at[c, half, i], a1_recv.at[c, half, i], line(half, i)[1]
                )
                copy.start()
                copies["a1"][c, half, i] = copy
        for i in (2, 1, 3):
            for half in (0, 1):
                block = rows.at[tp, span(c, half)]
                copy = remote(
                    block, block, a2_send.at[c, half, i, 0], a2_recv.at[c, half, i, 0], line(1 - half, i)[1]
                )
                copy.start()
                copies["a2"][c, half, i, 0] = copy

    def pass_on(c):
        for j in (1, 3, 2):
            for half in (0, 1):
                copies["a1"][c, half, j].wait_recv()
                source = line(half, SIDE - j)[0]
                block = rows.at[source, span(c, half)]
                for i in (2, 1, 3):
                    copy = remote(
                        block, block, a2_send.at[c, half, i, j], a2_recv.at[c, half, i, j], line(1 - half, i)[1]
                    )
                    copy.start()
                    copies["a2"][c, half, i, j] = copy

    for c in range(CHUNKS):
        known = EARLY + PER * c
        for j in range(len(counts), known):
            if j > 0:
                zs[j - 1].wait_recv()
        for j in range(len(counts), known):
            live = jnp.where(came[j].astype(F32) < DEAD / 2, 1.0, 0.0)
            n = jnp.sum(live, axis=0, keepdims=True)
            counts.append(n)
            starts.append(total)
            total = total + n
        for t in range(EARLY // PER):
            g = (c + t) * PER
            first, many = starts[g + PER - 1], counts[g + PER - 1]
            for k in range(PER - 2, -1, -1):
                first = jnp.where(lane_group == k, starts[g + k], first)
                many = jnp.where(lane_group == k, counts[g + k], many)
            place = jnp.where(lane_slot < many, first + lane_slot, -1.0)
            pick[:, t * WID : (t + 1) * WID] = jnp.where(
                down_rows + float(c * CHUNK) == place, 1.0, 0.0
            ).astype(BF)
        block = came[PER * c : PER * c + EARLY].reshape(EARLY * MOST, WID)
        rows[tp, c * CHUNK : (c + 1) * CHUNK] = jnp.dot(
            pick[...], block, preferred_element_type=F32
        ).astype(BF)
        begin_gather(c)
        if c > 0:
            pass_on(c - 1)
    pass_on(CHUNKS - 1)

    down_slots = lax.broadcasted_iota(jnp.int32, (MOST, WID), 0).astype(F32)
    lanes = lax.broadcasted_iota(jnp.int32, (MOST, WID), 1).astype(F32)
    for j in range(N_EP):
        place = jnp.where(down_slots < counts[j], starts[j] + down_slots, -1.0)
        for c in range(CHUNKS):
            spread[j * MOST : (j + 1) * MOST, c * WID : (c + 1) * WID] = jnp.where(
                lanes + float(c * CHUNK) == place, 1.0, 0.0
            ).astype(BF)
    for load in loads[3:]:
        load.wait()

    def compute(c):
        for half in (0, 1):
            for i in (1, 2, 3):
                for j in range(SIDE):
                    copies["a2"][c, half, i, j].wait_recv()
        at = slice(c * CHUNK, (c + 1) * CHUNK)
        chosen = jnp.concatenate([rows[k, at] for k in range(N_TP)], axis=1)
        both = jnp.dot(chosen, wgu[...], preferred_element_type=F32)
        gate, up = both[:, :WID], both[:, WID:]
        hidden = (gate / (1.0 + jnp.exp(-gate)) * up).astype(BF)
        partial = jnp.dot(hidden, wdb[...], preferred_element_type=F32).astype(BF)
        for k in range(N_TP):
            part[k // SIDE, k % SIDE, at] = partial[:, k * WID : (k + 1) * WID]

    def begin_sum(c):
        for i in (2, 1, 3):
            for half in (0, 1):
                t, peer = line(half, i)
                if half == 0:
                    block = part.at[:, t % SIDE, span(c, half)]
                else:
                    block = part.at[t // SIDE, :, span(c, half)]
                copy = remote(
                    block, got1.at[c, half, i - 1], r1_send.at[c, half, i], r1_recv.at[c, half, i], peer
                )
                copy.start()
                copies["r1"][c, half, i] = copy

    def go_on_sum(c):
        for half in (0, 1):
            for i in (1, 3, 2):
                copies["r1"][c, half, i].wait_recv()
            mine = part[:, x, span(c, half)] if half == 0 else part[y, :, span(c, half)]
            added = mine.astype(F32)
            for i in range(3):
                added = added + got1[c, half, i].astype(F32)
            sum1[c, half] = added.astype(BF)
            for i in (2, 1, 3):
                t, peer = line(1 - half, i)
                block = sum1.at[c, half, t // SIDE if half == 0 else t % SIDE]
                copy = remote(
                    block, got2.at[c, half, i - 1], r2_send.at[c, half, i], r2_recv.at[c, half, i], peer
                )
                copy.start()
                copies["r2"][c, half, i] = copy

    def end_sum(c):
        for half in (0, 1):
            for i in (1, 3, 2):
                copies["r2"][c, half, i].wait_recv()
            added = sum1[c, half, y if half == 0 else x].astype(F32)
            for i in range(3):
                added = added + got2[c, half, i].astype(F32)
            result[span(c, half)] = added.astype(BF)

    bs = {}

    def give_back(first, last):
        low = (min(first // PER, CHUNKS - 1) if first >= EARLY else 0) if first else 0
        low = max(0, (first - EARLY) // PER + 1) if first >= EARLY else 0
        slots = jnp.dot(
            spread[first * MOST : last * MOST, low * WID :], result[low * CHUNK :], preferred_element_type=F32
        ).astype(BF)
        back[first:last] = slots.reshape(last - first, MOST, WID)
        for i in range(last - 1, first - 1, -1):
            if i == 0:
                home[ep] = back[0]
                continue
            peer = ep_back(i)[1]
            copy = remote(back.at[i], home.at[ep], b_send.at[i], b_recv.at[i], peer)
            copy.start()
            bs[i] = copy

    for c in range(CHUNKS):
        compute(c)
        if c == 0:
            begin_sum(0)
    for c in SUM_ORDER[1:]:
        begin_sum(c)
    done, left = set(), N_EP
    for n, c in enumerate(SUM_ORDER):
        go_on_sum(c)
        if n > 0:
            before = SUM_ORDER[n - 1]
            end_sum(before)
            done.add(before)
            first = left
            while first > EARLY and all(k in done for k in range((first - 1 - EARLY) // PER + 1, CHUNKS)):
                first -= PER
            if first < left:
                give_back(first, left)
                left = first
    end_sum(SUM_ORDER[-1])
    give_back(0, left)

    for i in range(1, N_EP):
        bs[i].wait_recv()
    slots = home[...].reshape(N_EP * MOST, WID)
    out[...] = (
        jnp.dot(mix[0], slots, preferred_element_type=F32) + jnp.dot(mix[1], slots, preferred_element_type=F32)
    ).astype(BF)
    for copy in zs:
        copy.wait_send()
    for group in copies.values():
        for copy in group.values():
            copy.wait_send()
    for copy in bs.values():
        copy.wait_send()


def per_device(tokens, selected, affinity, w_gate, w_up, w_down):
    width = tokens.shape[1]
    dma = pltpu.SemaphoreType.DMA
    scratch = [
        pltpu.VMEM((2 * TOK, WID), BF),
        pltpu.VMEM((N_EP, MOST), jnp.int32),
        pltpu.VMEM((N_EP, MOST), F32),
        pltpu.VMEM((width, 2 * WID), BF),
        pltpu.VMEM((WID, width), BF),
        pltpu.VMEM((N_EP * MOST, 2 * TOK), BF),
        pltpu.VMEM((N_EP, MOST, WID), BF),
        pltpu.VMEM((N_EP, MOST, WID), BF),
        pltpu.VMEM((CHUNK, EARLY * MOST), BF),
        pltpu.VMEM((N_EP * MOST, ROWS), BF),
        pltpu.VMEM((N_TP, ROWS, WID), BF),
        pltpu.VMEM((SIDE, SIDE, ROWS, WID), BF),
        pltpu.VMEM((CHUNKS, 2, 3, SIDE, HALF, WID), BF),
        pltpu.VMEM((CHUNKS, 2, SIDE, HALF, WID), BF),
        pltpu.VMEM((CHUNKS, 2, 3, HALF, WID), BF),
        pltpu.VMEM((ROWS, WID), BF),
        pltpu.VMEM((N_EP, MOST, WID), BF),
        pltpu.VMEM((N_EP, MOST, WID), BF),
        pltpu.VMEM((2, TOK, N_EP * MOST), BF),
        dma((6,)),
        dma((N_EP,)),
        dma((N_EP,)),
        dma((CHUNKS, 2, 4)),
        dma((CHUNKS, 2, 4)),
        dma((CHUNKS, 2, 4, 4)),
        dma((CHUNKS, 2, 4, 4)),
        dma((CHUNKS, 2, 4)),
        dma((CHUNKS, 2, 4)),
        dma((CHUNKS, 2, 4)),
        dma((CHUNKS, 2, 4)),
        dma((N_EP,)),
        dma((N_EP,)),
    ]
    return pl.pallas_call(
        kernel,
        out_shape=jax.ShapeDtypeStruct((tokens.shape[0], WID), BF),
        in_specs=[pl.BlockSpec(memory_space=pl.ANY)] * 6,
        out_specs=pl.BlockSpec(memory_space=pltpu.VMEM),
        scratch_shapes=scratch,
        compiler_params=pltpu.CompilerParams(
            collective_id=0, has_side_effects=True, vmem_limit_bytes=48 * 1024 * 1024
        ),
    )(tokens, selected, affinity, w_gate[0], w_up[0], w_down[0])


def solution(mesh):
    return jax.shard_map(
        per_device,
        mesh=mesh,
        in_specs=(
            P("ep", None),
            P(None, "ep"),
            P(None, "ep"),
            P("ep", None, "tp"),
            P("ep", None, "tp"),
            P("ep", "tp", None),
        ),
        out_specs=P("ep", "tp"),
        check_vma=False,
    )
```

```python
import functools

import jax
import jax.numpy as jnp
from jax import lax
from jax.experimental import pallas as pl
from jax.experimental.pallas import tpu as pltpu
from jax.sharding import PartitionSpec as P

MESH = pl.DeviceIdType.MESH
BF = jnp.bfloat16
F32 = jnp.float32

N_EP, N_TP, N_Z, SIDE = 32, 16, 16, 4
MOST, TOK, WID = 32, 128, 128
ROWS = 512
EDGES = (0, 64, 192, 320, 448, 512)
CHUNKS = len(EDGES) - 1
LARGEST = 128
PER = WID // MOST
FULL = ROWS // MOST
TILES = 5
PAD = 2
DEAD = 1024.0

PLACES = [(0, 0), (0, 1)]
for _d in range(1, N_Z // 2):
    PLACES += [(_d, 0), (_d, 1), (N_Z - _d, 0), (N_Z - _d, 1)]
PLACES += [(N_Z // 2, 0), (N_Z // 2, 1)]
STEPS = ("Z0", "Z1", "F0", "Z2", "F1", "Z3", "F2", "Z4", "F3", "F4", "K0", "B0", "K1", "P", "K2", "K3", "K4", "B4", "S0", "B3", "S4", "B2", "S3", "E4", "B1", "S2", "E3", "S1", "E2", "E0", "E1")


def known_at(c):
    return N_EP - FULL + EDGES[c + 1] // MOST


def stage_of(i):
    return next(c for c in range(CHUNKS) if i < known_at(c))


def chunks_of(i):
    return [c for c in range(CHUNKS) if EDGES[c] // MOST <= i < known_at(c)]


def remote(src, dst, send, recv, device):
    return pltpu.make_async_remote_copy(
        src_ref=src, dst_ref=dst, send_sem=send, recv_sem=recv, device_id=device, device_id_type=MESH
    )


def kernel(
    tok, sel, aff, wg, wu, wd, out,
    tokb, selb, affb, wgu, wdb, onehot, sent, came, pick, spread, rows, part, got1, sum1, got2,
    result, back, home, mix,
    chain, in_sem, z_send, z_recv, a1_send, a1_recv, a2_send, a2_recv,
    r1_send, r1_recv, r2_send, r2_recv, b_send, b_recv,
):
    ep, tp = lax.axis_index("ep"), lax.axis_index("tp")
    z, core = ep // 2, ep % 2
    y, x = tp // SIDE, tp % SIDE

    def ep_peer(i):
        dz, dc = PLACES[i]
        e = lax.rem(z + dz, N_Z) * 2 + lax.rem(core + dc, 2)
        return e, {"ep": e, "tp": tp}

    def ep_back(i):
        dz, dc = PLACES[i]
        e = lax.rem(z + N_Z - dz, N_Z) * 2 + lax.rem(core + dc, 2)
        return e, {"ep": e, "tp": tp}

    def line(axis, i):
        if axis == 0:
            t = y * SIDE + lax.rem(x + i, SIDE)
        else:
            t = lax.rem(y + i, SIDE) * SIDE + x
        return t, {"ep": ep, "tp": t}

    loads = [
        pltpu.make_async_copy(sel, selb, in_sem.at[0]),
        pltpu.make_async_copy(aff, affb, in_sem.at[1]),
        pltpu.make_async_copy(
            tok.at[:, pl.ds(pl.multiple_of(tp * WID, WID), WID)], tokb.at[pl.ds(0, TOK)], in_sem.at[2]
        ),
        pltpu.make_async_copy(wg, wgu.at[:, pl.ds(0, WID)], in_sem.at[3]),
        pltpu.make_async_copy(wu, wgu.at[:, pl.ds(WID, WID)], in_sem.at[4]),
        pltpu.make_async_copy(wd, wdb, in_sem.at[5]),
    ]
    for load in loads:
        load.start()
    barrier = pltpu.get_barrier_semaphore()
    peers = [ep_peer(i)[1] for i in range(1, 6)]
    peers += [line(a, i)[1] for a in (0, 1) for i in (1, 2, 3)]
    for peer in peers:
        pl.semaphore_signal(barrier, inc=1, device_id=peer, device_id_type=MESH)

    tokb[TOK : 2 * TOK] = jnp.full((TOK, WID), DEAD, BF)
    loads[0].wait()
    loads[1].wait()
    sel_t = selb[...].astype(F32).T
    aff_t = affb[...].T
    lane2 = lax.broadcasted_iota(jnp.int32, (MOST, 2 * TOK), 1).astype(F32)
    lane1 = lax.broadcasted_iota(jnp.int32, (MOST, TOK), 1).astype(F32)
    for e in range(N_EP):
        column = sel_t[:, e : e + 1]
        spot = jnp.where(column < 0.0, float(TOK), column)
        onehot[e * MOST : (e + 1) * MOST] = jnp.where(lane2 == spot, 1.0, 0.0).astype(BF)
    loads[2].wait()
    sent[...] = (
        jnp.dot(onehot[...], tokb[...], preferred_element_type=F32).astype(BF).reshape(N_EP, MOST, WID)
    )
    came[PAD] = sent[ep]
    came[:PAD] = jnp.zeros((PAD, MOST, WID), BF)
    result[...] = jnp.zeros_like(result)
    with jax.named_scope("barrier"):
        pl.semaphore_wait(barrier, len(peers))

    def send_to(ds):
        for i in range(1, N_EP):
            if min(PLACES[i][0], N_Z - PLACES[i][0]) in ds:
                e, peer = ep_peer(i)
                remote(sent.at[e], came.at[PAD + i], z_send.at[0], z_recv.at[stage_of(i)], peer).start()

    def tell(n, k):
        for steps in (n, N_Z - n):
            there = {"ep": lax.rem(ep + 2 * steps, N_EP), "tp": tp}
            pl.semaphore_signal(chain.at[k], inc=1, device_id=there, device_id_type=MESH)

    def told(k):
        with jax.named_scope("chain"):
            pl.semaphore_wait(chain.at[k], 2)

    tell(1, 0)
    send_to((0, 1))
    told(0)
    tell(2, 1)
    send_to((2,))
    told(1)
    tell(2, 2)
    tell(4, 3)
    send_to((3, 4))
    told(2)
    send_to((5, 6))
    told(3)
    send_to((7, 8))

    for q in range(N_EP * MOST // TOK):
        tall = []
        for e in range(q * PER, (q + 1) * PER):
            tall.append(jnp.where(lane1 == sel_t[:, e : e + 1], aff_t[:, e : e + 1], 0.0))
        wide = jnp.concatenate(tall, axis=0).T
        high = wide.astype(BF)
        mix[0, :, q * TOK : (q + 1) * TOK] = high
        mix[1, :, q * TOK : (q + 1) * TOK] = (wide - high.astype(F32)).astype(BF)

    lane_row = lax.broadcasted_iota(jnp.int32, (1, WID), 1)
    lane_slot = lax.rem(lane_row, MOST).astype(F32)
    lane_group = lane_row // MOST

    starts, counts = [], []
    total = jnp.zeros((1, WID), F32)
    gathers = {}

    def wait_for(block, semaphore):
        pltpu.make_async_copy(block, block, semaphore).wait()

    def span(c, half):
        n = (EDGES[c + 1] - EDGES[c]) // 2
        return pl.ds(EDGES[c] + half * n, n)

    def first_half(c):
        return pl.ds(0, (EDGES[c + 1] - EDGES[c]) // 2)

    def begin_gather(c):
        for i in (2, 1, 3):
            for half in (0, 1):
                block = rows.at[tp, span(c, half)]
                copy = remote(
                    block, block, a1_send.at[0], a1_recv.at[c, half, i], line(half, i)[1]
                )
                copy.start()
                gathers[c, half, i] = copy
        for i in (2, 1, 3):
            for half in (0, 1):
                block = rows.at[tp, span(c, half)]
                remote(block, block, a2_send.at[0], a2_recv.at[c], line(1 - half, i)[1]).start()

    def pick_rows(c):
        nonlocal total
        low, high = EDGES[c], EDGES[c + 1]
        before, known = len(counts), known_at(c)
        with jax.named_scope("zwait"):
            new = max(before, 1)
            wait_for(came.at[pl.ds(PAD + new, known - new)], z_recv.at[c])
        for j in range(before, known):
            live = jnp.where(came[PAD + j].astype(F32) < DEAD / 2, 1.0, 0.0)
            n = jnp.sum(live, axis=0, keepdims=True)
            counts.append(n)
            starts.append(total)
            total = total + n
        down_rows = lax.broadcasted_iota(jnp.int32, (high - low, WID), 0).astype(F32) + float(low)
        none = jnp.zeros((1, WID), F32)
        for t in range(TILES):
            first, many = none, none
            for k in range(PER):
                j = known - TILES * PER + t * PER + k
                first = jnp.where(lane_group == k, starts[j] if j >= 0 else none, first)
                many = jnp.where(lane_group == k, counts[j] if j >= 0 else none, many)
            place = jnp.where(lane_slot < many, first + lane_slot, -1.0)
            pick[: high - low, t * WID : (t + 1) * WID] = jnp.where(down_rows == place, 1.0, 0.0).astype(BF)
        block = came[PAD + known - TILES * PER : PAD + known].reshape(TILES * WID, WID)
        rows[tp, low:high] = jnp.dot(pick[: high - low], block, preferred_element_type=F32).astype(BF)
        begin_gather(c)

    def pass_on(c):
        for j in (1, 3, 2):
            for half in (0, 1):
                with jax.named_scope("pass_wait"):
                    gathers[c, half, j].wait_recv()
                source = line(half, SIDE - j)[0]
                block = rows.at[source, span(c, half)]
                for i in (2, 1, 3):
                    remote(block, block, a2_send.at[0], a2_recv.at[c], line(1 - half, i)[1]).start()

    def place_rows(_):
        down_slots = lax.broadcasted_iota(jnp.int32, (MOST, WID), 0).astype(F32)
        lanes = lax.broadcasted_iota(jnp.int32, (MOST, WID), 1).astype(F32)
        for j in range(N_EP):
            place = jnp.where(down_slots < counts[j], starts[j] + down_slots, -1.0)
            for q in range(ROWS // WID):
                spread[j * MOST : (j + 1) * MOST, q * WID : (q + 1) * WID] = jnp.where(
                    lanes + float(q * WID) == place, 1.0, 0.0
                ).astype(BF)

    def compute(c):
        with jax.named_scope("gather_wait"):
            wait_for(rows.at[pl.ds(0, N_TP - SIDE), pl.ds(EDGES[c], EDGES[c + 1] - EDGES[c])], a2_recv.at[c])
        if c == 0:
            for load in loads[3:]:
                load.wait()
        at = slice(EDGES[c], EDGES[c + 1])
        chosen = jnp.concatenate([rows[k, at] for k in range(N_TP)], axis=1)
        both = jnp.dot(chosen, wgu[...], preferred_element_type=F32)
        gate, up = both[:, :WID], both[:, WID:]
        hidden = (gate / (1.0 + jnp.exp(-gate)) * up).astype(BF)
        partial = jnp.dot(hidden, wdb[...], preferred_element_type=F32).astype(BF)
        for k in range(N_TP):
            part[k // SIDE, k % SIDE, at] = partial[:, k * WID : (k + 1) * WID]

    def begin_sum(c):
        for i in (2, 1, 3):
            for half in (0, 1):
                t, peer = line(half, i)
                if half == 0:
                    block = part.at[:, t % SIDE, span(c, half)]
                else:
                    block = part.at[t // SIDE, :, span(c, half)]
                there = got1.at[c, half, i - 1, :, first_half(c)]
                remote(block, there, r1_send.at[0], r1_recv.at[c, half], peer).start()

    def go_on_sum(c):
        for half in (0, 1):
            with jax.named_scope("sum1_wait"):
                wait_for(got1.at[c, half, :, :, first_half(c)], r1_recv.at[c, half])
            mine = part[:, x, span(c, half)] if half == 0 else part[y, :, span(c, half)]
            added = mine.astype(F32)
            for i in range(3):
                added = added + got1[c, half, i, :, first_half(c)].astype(F32)
            sum1[c, half, :, first_half(c)] = added.astype(BF)
            for i in (2, 1, 3):
                t, peer = line(1 - half, i)
                block = sum1.at[c, half, t // SIDE if half == 0 else t % SIDE, first_half(c)]
                remote(block, got2.at[c, half, i - 1, first_half(c)], r2_send.at[0], r2_recv.at[c], peer).start()

    done, left = set(), list(range(N_EP))

    def give_back(js):
        first, last = js[0], js[-1] + 1
        low = EDGES[chunks_of(first)[0]] // WID * WID
        high = -(-EDGES[chunks_of(js[-1])[-1] + 1] // WID) * WID
        slots = jnp.dot(
            spread[first * MOST : last * MOST, low:high],
            result[low:high],
            preferred_element_type=F32,
        ).astype(BF)
        back[first:last] = slots.reshape(last - first, MOST, WID)
        for i in reversed(js):
            if i == 0:
                home[ep] = back[0]
            else:
                remote(back.at[i], home.at[ep], b_send.at[0], b_recv.at[0], ep_back(i)[1]).start()

    def end_sum(c):
        with jax.named_scope("sum2_wait"):
            wait_for(got2.at[c, :, :, first_half(c)], r2_recv.at[c])
        for half in (0, 1):
            added = sum1[c, half, y if half == 0 else x, first_half(c)].astype(F32)
            for i in range(3):
                added = added + got2[c, half, i, first_half(c)].astype(F32)
            result[span(c, half)] = added.astype(BF)
        done.add(c)
        ready = [i for i in left if done.issuperset(chunks_of(i))]
        runs = []
        for i in ready:
            left.remove(i)
            if runs and runs[-1][-1] == i - 1:
                runs[-1].append(i)
            else:
                runs.append([i])
        for js in reversed(runs):
            give_back(js)

    steps = {
        "Z": pick_rows,
        "F": pass_on,
        "P": place_rows,
        "K": compute,
        "B": begin_sum,
        "S": go_on_sum,
        "E": end_sum,
    }
    for step in STEPS:
        steps[step[0]](int(step[1:] or 0))

    wait_for(sent.at[pl.ds(1, N_EP - 1)], z_send.at[0])
    wait_for(rows.at[pl.ds(0, 3)], a1_send.at[0])
    wait_for(rows.at[pl.ds(0, 12)], a2_send.at[0])
    wait_for(rows.at[pl.ds(0, 12)], r1_send.at[0])
    wait_for(rows.at[pl.ds(0, 3)], r2_send.at[0])
    wait_for(back.at[pl.ds(1, N_EP - 1)], b_send.at[0])
    with jax.named_scope("home_wait"):
        wait_for(home.at[pl.ds(1, N_EP - 1)], b_recv.at[0])
    slots = home[...].reshape(N_EP * MOST, WID)
    out[...] = (
        jnp.dot(mix[0], slots, preferred_element_type=F32) + jnp.dot(mix[1], slots, preferred_element_type=F32)
    ).astype(BF)


def per_device(tokens, selected, affinity, w_gate, w_up, w_down):
    width = tokens.shape[1]
    dma = pltpu.SemaphoreType.DMA
    scratch = [
        pltpu.VMEM((2 * TOK, WID), BF),
        pltpu.VMEM((N_EP, MOST), jnp.int32),
        pltpu.VMEM((N_EP, MOST), F32),
        pltpu.VMEM((width, 2 * WID), BF),
        pltpu.VMEM((WID, width), BF),
        pltpu.VMEM((N_EP * MOST, 2 * TOK), BF),
        pltpu.VMEM((N_EP, MOST, WID), BF),
        pltpu.VMEM((PAD + N_EP, MOST, WID), BF),
        pltpu.VMEM((LARGEST, TILES * WID), BF),
        pltpu.VMEM((N_EP * MOST, ROWS), BF),
        pltpu.VMEM((N_TP, ROWS, WID), BF),
        pltpu.VMEM((SIDE, SIDE, ROWS, WID), BF),
        pltpu.VMEM((CHUNKS, 2, 3, SIDE, LARGEST // 2, WID), BF),
        pltpu.VMEM((CHUNKS, 2, SIDE, LARGEST // 2, WID), BF),
        pltpu.VMEM((CHUNKS, 2, 3, LARGEST // 2, WID), BF),
        pltpu.VMEM((ROWS, WID), BF),
        pltpu.VMEM((N_EP, MOST, WID), BF),
        pltpu.VMEM((N_EP, MOST, WID), BF),
        pltpu.VMEM((2, TOK, N_EP * MOST), BF),
        pltpu.SemaphoreType.REGULAR((4,)),
        dma((6,)),
        dma((1,)),
        dma((CHUNKS,)),
        dma((1,)),
        dma((CHUNKS, 2, 4)),
        dma((1,)),
        dma((CHUNKS,)),
        dma((1,)),
        dma((CHUNKS, 2)),
        dma((1,)),
        dma((CHUNKS,)),
        dma((1,)),
        dma((1,)),
    ]
    return pl.pallas_call(
        kernel,
        out_shape=jax.ShapeDtypeStruct((tokens.shape[0], WID), BF),
        in_specs=[pl.BlockSpec(memory_space=pl.ANY)] * 6,
        out_specs=pl.BlockSpec(memory_space=pltpu.VMEM),
        scratch_shapes=scratch,
        compiler_params=pltpu.CompilerParams(
            collective_id=0, has_side_effects=True, vmem_limit_bytes=67043328
        ),
    )(tokens, selected, affinity, w_gate[0], w_up[0], w_down[0])


def solution(mesh):
    return jax.shard_map(
        per_device,
        mesh=mesh,
        in_specs=(
            P("ep", None),
            P(None, "ep"),
            P(None, "ep"),
            P("ep", None, "tp"),
            P("ep", None, "tp"),
            P("ep", "tp", None),
        ),
        out_specs=P("ep", "tp"),
        check_vma=False,
    )
```

```python
import functools

import jax
import jax.numpy as jnp
from jax import lax
from jax.experimental import pallas as pl
from jax.experimental.pallas import tpu as pltpu
from jax.sharding import PartitionSpec as P

MESH = pl.DeviceIdType.MESH
BF = jnp.bfloat16
F32 = jnp.float32

N_EP, N_TP, N_Z, SIDE = 32, 16, 16, 4
MOST, TOK, WID = 32, 128, 128
ROWS = 512
EDGES = (0, 64, 192, 320, 448, 512)
CHUNKS = len(EDGES) - 1
LARGEST = max(b - a for a, b in zip(EDGES, EDGES[1:]))
PER = WID // MOST
FULL = ROWS // MOST
TILES = -(-(LARGEST // MOST + FULL) // PER)
PAD = max(0, TILES * PER - (N_EP - FULL + EDGES[1] // MOST))
DEAD = 1024.0

PLACES = [(0, 0), (0, 1)]
for _d in range(1, N_Z // 2):
    PLACES += [(_d, 0), (_d, 1), (N_Z - _d, 0), (N_Z - _d, 1)]
PLACES += [(N_Z // 2, 0), (N_Z // 2, 1)]
STEPS = ("Z0", "Z1", "F0", "Z2", "F1", "Z3", "F2", "Z4", "F3", "F4", "K0", "B0", "K1", "P", "K2", "K3", "K4", "B4", "S0", "B3", "S4", "B2", "S3", "E4", "B1", "S2", "E3", "S1", "E2", "E0", "E1")


def known_at(c):
    return N_EP - FULL + EDGES[c + 1] // MOST


def stage_of(i):
    return next(c for c in range(CHUNKS) if i < known_at(c))


def chunks_of(i):
    return [c for c in range(CHUNKS) if EDGES[c] // MOST <= i < known_at(c)]


def remote(src, dst, send, recv, device):
    return pltpu.make_async_remote_copy(
        src_ref=src, dst_ref=dst, send_sem=send, recv_sem=recv, device_id=device, device_id_type=MESH
    )


def kernel(
    tok, sel, aff, wg, wu, wd, out,
    tokb, selb, affb, wgu, wdb, onehot, sent, came, pick, spread, rows, part, got1, sum1, got2,
    result, back, home, mix,
    chain, in_sem, z_send, z_recv, a1_send, a1_recv, a2_send, a2_recv,
    r1_send, r1_recv, r2_send, r2_recv, b_send, b_recv,
):
    ep, tp = lax.axis_index("ep"), lax.axis_index("tp")
    z, core = ep // 2, ep % 2
    y, x = tp // SIDE, tp % SIDE

    def ep_peer(i):
        dz, dc = PLACES[i]
        e = lax.rem(z + dz, N_Z) * 2 + lax.rem(core + dc, 2)
        return e, {"ep": e, "tp": tp}

    def ep_back(i):
        dz, dc = PLACES[i]
        e = lax.rem(z + N_Z - dz, N_Z) * 2 + lax.rem(core + dc, 2)
        return e, {"ep": e, "tp": tp}

    def line(axis, i):
        if axis == 0:
            t = y * SIDE + lax.rem(x + i, SIDE)
        else:
            t = lax.rem(y + i, SIDE) * SIDE + x
        return t, {"ep": ep, "tp": t}

    loads = [
        pltpu.make_async_copy(sel, selb, in_sem.at[0]),
        pltpu.make_async_copy(aff, affb, in_sem.at[1]),
        pltpu.make_async_copy(
            tok.at[:, pl.ds(pl.multiple_of(tp * WID, WID), WID)], tokb.at[pl.ds(0, TOK)], in_sem.at[2]
        ),
        pltpu.make_async_copy(wg, wgu.at[:, pl.ds(0, WID)], in_sem.at[3]),
        pltpu.make_async_copy(wu, wgu.at[:, pl.ds(WID, WID)], in_sem.at[4]),
        pltpu.make_async_copy(wd, wdb, in_sem.at[5]),
    ]
    for load in loads:
        load.start()
    barrier = pltpu.get_barrier_semaphore()
    peers = [ep_peer(i)[1] for i in range(1, 10)]
    peers += [line(a, i)[1] for a in (0, 1) for i in (1, 2, 3)]
    for peer in peers:
        pl.semaphore_signal(barrier, inc=1, device_id=peer, device_id_type=MESH)

    tokb[TOK : 2 * TOK] = jnp.full((TOK, WID), DEAD, BF)
    for load in loads[:3]:
        load.wait()
    with jax.named_scope("barrier"):
        pl.semaphore_wait(barrier, len(peers))

    def tell(n, k):
        for steps in (n, N_Z - n):
            there = {"ep": lax.rem(ep + 2 * steps, N_EP), "tp": tp}
            pl.semaphore_signal(chain.at[k], inc=1, device_id=there, device_id_type=MESH)

    def told(k):
        with jax.named_scope("chain"):
            pl.semaphore_wait(chain.at[k], 2)

    tell(2, 0)
    sel_t = selb[...].astype(F32).T
    aff_t = affb[...].T
    lane2 = lax.broadcasted_iota(jnp.int32, (MOST, 2 * TOK), 1).astype(F32)
    lane1 = lax.broadcasted_iota(jnp.int32, (MOST, TOK), 1).astype(F32)
    for e in range(N_EP):
        column = sel_t[:, e : e + 1]
        spot = jnp.where(column < 0.0, float(TOK), column)
        onehot[e * MOST : (e + 1) * MOST] = jnp.where(lane2 == spot, 1.0, 0.0).astype(BF)
    sent[...] = (
        jnp.dot(onehot[...], tokb[...], preferred_element_type=F32).astype(BF).reshape(N_EP, MOST, WID)
    )

    def send_to(ds):
        for i in range(1, N_EP):
            if min(PLACES[i][0], N_Z - PLACES[i][0]) in ds:
                e, peer = ep_peer(i)
                remote(sent.at[e], came.at[PAD + i], z_send.at[0], z_recv.at[stage_of(i)], peer).start()

    send_to((0, 1, 2))
    told(0)
    tell(2, 1)
    tell(4, 2)
    send_to((3, 4))
    told(1)
    send_to((5, 6))
    told(2)
    send_to((7, 8))
    came[PAD] = sent[ep]
    if PAD:
        came[:PAD] = jnp.zeros((PAD, MOST, WID), BF)
    result[...] = jnp.zeros_like(result)

    for q in range(N_EP * MOST // TOK):
        tall = []
        for e in range(q * PER, (q + 1) * PER):
            tall.append(jnp.where(lane1 == sel_t[:, e : e + 1], aff_t[:, e : e + 1], 0.0))
        wide = jnp.concatenate(tall, axis=0).T
        high = wide.astype(BF)
        mix[:TOK, q * TOK : (q + 1) * TOK] = high
        mix[TOK:, q * TOK : (q + 1) * TOK] = (wide - high.astype(F32)).astype(BF)

    lane_row = lax.broadcasted_iota(jnp.int32, (1, WID), 1)
    lane_slot = lax.rem(lane_row, MOST).astype(F32)
    lane_group = lane_row // MOST

    starts, counts = [], []
    total = jnp.zeros((1, WID), F32)
    gathers = {}

    def wait_for(block, semaphore):
        pltpu.make_async_copy(block, block, semaphore).wait()

    def span(c, half):
        n = (EDGES[c + 1] - EDGES[c]) // 2
        return pl.ds(EDGES[c] + half * n, n)

    def first_half(c):
        return pl.ds(0, (EDGES[c + 1] - EDGES[c]) // 2)

    def begin_gather(c):
        for i in (2, 1, 3):
            for half in (0, 1):
                block = rows.at[tp, span(c, half)]
                copy = remote(
                    block, block, a1_send.at[0], a1_recv.at[c, half, i], line(half, i)[1]
                )
                copy.start()
                gathers[c, half, i] = copy
        for i in (2, 1, 3):
            for half in (0, 1):
                block = rows.at[tp, span(c, half)]
                remote(block, block, a2_send.at[0], a2_recv.at[c], line(1 - half, i)[1]).start()

    def pick_rows(c):
        nonlocal total
        low, high = EDGES[c], EDGES[c + 1]
        before, known = len(counts), known_at(c)
        with jax.named_scope("zwait"):
            new = max(before, 1)
            wait_for(came.at[pl.ds(PAD + new, known - new)], z_recv.at[c])
        for j in range(before, known):
            live = jnp.where(came[PAD + j].astype(F32) < DEAD / 2, 1.0, 0.0)
            n = jnp.sum(live, axis=0, keepdims=True)
            counts.append(n)
            starts.append(total)
            total = total + n
        down_rows = lax.broadcasted_iota(jnp.int32, (high - low, WID), 0).astype(F32) + float(low)
        none = jnp.zeros((1, WID), F32)
        for t in range(TILES):
            first, many = none, none
            for k in range(PER):
                j = known - TILES * PER + t * PER + k
                first = jnp.where(lane_group == k, starts[j] if j >= 0 else none, first)
                many = jnp.where(lane_group == k, counts[j] if j >= 0 else none, many)
            place = jnp.where(lane_slot < many, first + lane_slot, -1.0)
            pick[: high - low, t * WID : (t + 1) * WID] = jnp.where(down_rows == place, 1.0, 0.0).astype(BF)
        block = came[PAD + known - TILES * PER : PAD + known].reshape(TILES * WID, WID)
        rows[tp, low:high] = jnp.dot(pick[: high - low], block, preferred_element_type=F32).astype(BF)
        begin_gather(c)

    def pass_on(c):
        for j in (1, 3, 2):
            for half in (0, 1):
                with jax.named_scope("pass_wait"):
                    gathers[c, half, j].wait_recv()
                source = line(half, SIDE - j)[0]
                block = rows.at[source, span(c, half)]
                for i in (2, 1, 3):
                    remote(block, block, a2_send.at[0], a2_recv.at[c], line(1 - half, i)[1]).start()

    def place_rows(_):
        down_slots = lax.broadcasted_iota(jnp.int32, (MOST, WID), 0).astype(F32)
        lanes = lax.broadcasted_iota(jnp.int32, (MOST, WID), 1).astype(F32)
        for j in range(N_EP):
            place = jnp.where(down_slots < counts[j], starts[j] + down_slots, -1.0)
            for q in range(ROWS // WID):
                spread[j * MOST : (j + 1) * MOST, q * WID : (q + 1) * WID] = jnp.where(
                    lanes + float(q * WID) == place, 1.0, 0.0
                ).astype(BF)

    def compute(c):
        with jax.named_scope("gather_wait"):
            wait_for(rows.at[pl.ds(0, N_TP - SIDE), pl.ds(EDGES[c], EDGES[c + 1] - EDGES[c])], a2_recv.at[c])
        if c == 0:
            for load in loads[3:]:
                load.wait()
        at = slice(EDGES[c], EDGES[c + 1])
        chosen = jnp.concatenate([rows[k, at] for k in range(N_TP)], axis=1)
        both = jnp.dot(chosen, wgu[...], preferred_element_type=F32)
        gate, up = both[:, :WID], both[:, WID:]
        hidden = (gate / (1.0 + jnp.exp(-gate)) * up).astype(BF)
        partial = jnp.dot(hidden, wdb[...], preferred_element_type=F32).astype(BF)
        for k in range(N_TP):
            part[k // SIDE, k % SIDE, at] = partial[:, k * WID : (k + 1) * WID]

    def begin_sum(c):
        for i in (2, 1, 3):
            for half in (0, 1):
                t, peer = line(half, i)
                if half == 0:
                    block = part.at[:, t % SIDE, span(c, half)]
                else:
                    block = part.at[t // SIDE, :, span(c, half)]
                there = got1.at[c, half, i - 1, :, first_half(c)]
                remote(block, there, r1_send.at[0], r1_recv.at[c, half], peer).start()

    def go_on_sum(c):
        for half in (0, 1):
            with jax.named_scope("sum1_wait"):
                wait_for(got1.at[c, half, :, :, first_half(c)], r1_recv.at[c, half])
            mine = part[:, x, span(c, half)] if half == 0 else part[y, :, span(c, half)]
            added = mine.astype(F32)
            for i in range(3):
                added = added + got1[c, half, i, :, first_half(c)].astype(F32)
            sum1[c, half, :, first_half(c)] = added.astype(BF)
            for i in (2, 1, 3):
                t, peer = line(1 - half, i)
                block = sum1.at[c, half, t // SIDE if half == 0 else t % SIDE, first_half(c)]
                remote(block, got2.at[c, half, i - 1, first_half(c)], r2_send.at[0], r2_recv.at[c], peer).start()

    done, left = set(), list(range(N_EP))

    def give_back(js):
        first, last = js[0], js[-1] + 1
        low = EDGES[chunks_of(first)[0]] // WID * WID
        high = -(-EDGES[chunks_of(js[-1])[-1] + 1] // WID) * WID
        slots = jnp.dot(
            spread[first * MOST : last * MOST, low:high],
            result[low:high],
            preferred_element_type=F32,
        ).astype(BF)
        back[first:last] = slots.reshape(last - first, MOST, WID)
        for i in reversed(js):
            if i == 0:
                home[ep] = back[0]
            else:
                remote(back.at[i], home.at[ep], b_send.at[0], b_recv.at[0], ep_back(i)[1]).start()

    def end_sum(c):
        with jax.named_scope("sum2_wait"):
            wait_for(got2.at[c, :, :, first_half(c)], r2_recv.at[c])
        for half in (0, 1):
            added = sum1[c, half, y if half == 0 else x, first_half(c)].astype(F32)
            for i in range(3):
                added = added + got2[c, half, i, first_half(c)].astype(F32)
            result[span(c, half)] = added.astype(BF)
        done.add(c)
        ready = [i for i in left if done.issuperset(chunks_of(i))]
        runs = []
        for i in ready:
            left.remove(i)
            if runs and runs[-1][-1] == i - 1 and len(runs[-1]) < MOST // 4:
                runs[-1].append(i)
            else:
                runs.append([i])
        for js in reversed(runs):
            give_back(js)

    steps = {
        "Z": pick_rows,
        "F": pass_on,
        "P": place_rows,
        "K": compute,
        "B": begin_sum,
        "S": go_on_sum,
        "E": end_sum,
    }
    for step in STEPS:
        steps[step[0]](int(step[1:] or 0))

    wait_for(sent.at[pl.ds(1, N_EP - 1)], z_send.at[0])
    wait_for(rows.at[pl.ds(0, 3)], a1_send.at[0])
    wait_for(rows.at[pl.ds(0, 12)], a2_send.at[0])
    wait_for(rows.at[pl.ds(0, 12)], r1_send.at[0])
    wait_for(rows.at[pl.ds(0, 3)], r2_send.at[0])
    wait_for(back.at[pl.ds(1, N_EP - 1)], b_send.at[0])
    with jax.named_scope("home_wait"):
        wait_for(home.at[pl.ds(1, N_EP - 1)], b_recv.at[0])
    slots = home[...].reshape(N_EP * MOST, WID)
    weighted = jnp.dot(mix[...], slots, preferred_element_type=F32)
    out[...] = (weighted[:TOK] + weighted[TOK:]).astype(BF)


def per_device(tokens, selected, affinity, w_gate, w_up, w_down):
    width = tokens.shape[1]
    dma = pltpu.SemaphoreType.DMA
    scratch = [
        pltpu.VMEM((2 * TOK, WID), BF),
        pltpu.VMEM((N_EP, MOST), jnp.int32),
        pltpu.VMEM((N_EP, MOST), F32),
        pltpu.VMEM((width, 2 * WID), BF),
        pltpu.VMEM((WID, width), BF),
        pltpu.VMEM((N_EP * MOST, 2 * TOK), BF),
        pltpu.VMEM((N_EP, MOST, WID), BF),
        pltpu.VMEM((PAD + N_EP, MOST, WID), BF),
        pltpu.VMEM((LARGEST, TILES * WID), BF),
        pltpu.VMEM((N_EP * MOST, ROWS), BF),
        pltpu.VMEM((N_TP, ROWS, WID), BF),
        pltpu.VMEM((SIDE, SIDE, ROWS, WID), BF),
        pltpu.VMEM((CHUNKS, 2, 3, SIDE, LARGEST // 2, WID), BF),
        pltpu.VMEM((CHUNKS, 2, SIDE, LARGEST // 2, WID), BF),
        pltpu.VMEM((CHUNKS, 2, 3, LARGEST // 2, WID), BF),
        pltpu.VMEM((ROWS, WID), BF),
        pltpu.VMEM((N_EP, MOST, WID), BF),
        pltpu.VMEM((N_EP, MOST, WID), BF),
        pltpu.VMEM((2 * TOK, N_EP * MOST), BF),
        pltpu.SemaphoreType.REGULAR((3,)),
        dma((6,)),
        dma((1,)),
        dma((CHUNKS,)),
        dma((1,)),
        dma((CHUNKS, 2, 4)),
        dma((1,)),
        dma((CHUNKS,)),
        dma((1,)),
        dma((CHUNKS, 2)),
        dma((1,)),
        dma((CHUNKS,)),
        dma((1,)),
        dma((1,)),
    ]
    return pl.pallas_call(
        kernel,
        out_shape=jax.ShapeDtypeStruct((tokens.shape[0], WID), BF),
        in_specs=[pl.BlockSpec(memory_space=pl.ANY)] * 6,
        out_specs=pl.BlockSpec(memory_space=pltpu.VMEM),
        scratch_shapes=scratch,
        compiler_params=pltpu.CompilerParams(
            collective_id=0, has_side_effects=True, vmem_limit_bytes=67043328
        ),
    )(tokens, selected, affinity, w_gate[0], w_up[0], w_down[0])


def solution(mesh):
    return jax.shard_map(
        per_device,
        mesh=mesh,
        in_specs=(
            P("ep", None),
            P(None, "ep"),
            P(None, "ep"),
            P("ep", None, "tp"),
            P("ep", None, "tp"),
            P("ep", "tp", None),
        ),
        out_specs=P("ep", "tp"),
        check_vma=False,
    )
```

```python
import functools

import jax
import jax.numpy as jnp
from jax import lax
from jax.experimental import pallas as pl
from jax.experimental.pallas import tpu as pltpu
from jax.sharding import PartitionSpec as P

MESH = pl.DeviceIdType.MESH
BF = jnp.bfloat16
F32 = jnp.float32

N_EP, N_TP, N_Z, SIDE = 32, 16, 16, 4
MOST, TOK, WID = 32, 128, 128
ROWS = 512
EDGES = (0, 64, 160, 288, 416, 512)
CHUNKS = len(EDGES) - 1
LARGEST = max(b - a for a, b in zip(EDGES, EDGES[1:]))
PER = WID // MOST
FULL = ROWS // MOST
TILES = -(-(LARGEST // MOST + FULL) // PER)
PAD = max(0, TILES * PER - (N_EP - FULL + EDGES[1] // MOST))
DEAD = 1024.0

PLACES = [(0, 0), (0, 1)]
for _d in range(1, N_Z // 2):
    PLACES += [(_d, 0), (_d, 1), (N_Z - _d, 0), (N_Z - _d, 1)]
PLACES += [(N_Z // 2, 0), (N_Z // 2, 1)]
STEPS = ("Z0", "Z1", "F0", "Z2", "F1", "Z3", "F2", "Z4", "F3", "F4", "K0", "B0", "K1", "P", "K2", "K3", "K4", "B4", "S0", "B3", "S4", "B2", "S3", "E4", "B1", "S2", "E3", "S1", "E2", "E0", "E1")


def known_at(c):
    return N_EP - FULL + EDGES[c + 1] // MOST


def stage_of(i):
    return next(c for c in range(CHUNKS) if i < known_at(c))


def chunks_of(i):
    return [c for c in range(CHUNKS) if EDGES[c] // MOST <= i < known_at(c)]


def remote(src, dst, send, recv, device):
    return pltpu.make_async_remote_copy(
        src_ref=src, dst_ref=dst, send_sem=send, recv_sem=recv, device_id=device, device_id_type=MESH
    )


def kernel(
    tok, sel, aff, wg, wu, wd, out,
    tokb, selb, affb, wgu, wdb, onehot, sent, came, pick, spread, rows, part, got1, sum1, got2,
    result, back, home, mix,
    chain, in_sem, z_send, z_recv, a1_send, a1_recv, a2_send, a2_recv,
    r1_send, r1_recv, r2_send, r2_recv, b_send, b_recv,
):
    ep, tp = lax.axis_index("ep"), lax.axis_index("tp")
    z, core = ep // 2, ep % 2
    y, x = tp // SIDE, tp % SIDE

    def ep_peer(i):
        dz, dc = PLACES[i]
        e = lax.rem(z + dz, N_Z) * 2 + lax.rem(core + dc, 2)
        return e, {"ep": e, "tp": tp}

    def ep_back(i):
        dz, dc = PLACES[i]
        e = lax.rem(z + N_Z - dz, N_Z) * 2 + lax.rem(core + dc, 2)
        return e, {"ep": e, "tp": tp}

    def line(axis, i):
        if axis == 0:
            t = y * SIDE + lax.rem(x + i, SIDE)
        else:
            t = lax.rem(y + i, SIDE) * SIDE + x
        return t, {"ep": ep, "tp": t}

    loads = [
        pltpu.make_async_copy(sel, selb, in_sem.at[0]),
        pltpu.make_async_copy(aff, affb, in_sem.at[1]),
        pltpu.make_async_copy(
            tok.at[:, pl.ds(pl.multiple_of(tp * WID, WID), WID)], tokb.at[pl.ds(0, TOK)], in_sem.at[2]
        ),
        pltpu.make_async_copy(wg, wgu.at[:, pl.ds(0, WID)], in_sem.at[3]),
        pltpu.make_async_copy(wu, wgu.at[:, pl.ds(WID, WID)], in_sem.at[4]),
        pltpu.make_async_copy(wd, wdb, in_sem.at[5]),
    ]
    for load in loads:
        load.start()
    barrier = pltpu.get_barrier_semaphore()
    peers = [ep_peer(i)[1] for i in range(1, 10)]
    peers += [line(a, i)[1] for a in (0, 1) for i in (1, 2, 3)]
    for peer in peers:
        pl.semaphore_signal(barrier, inc=1, device_id=peer, device_id_type=MESH)

    tokb[TOK : 2 * TOK] = jnp.full((TOK, WID), DEAD, BF)
    for load in loads[:3]:
        load.wait()
    with jax.named_scope("barrier"):
        pl.semaphore_wait(barrier, len(peers))

    def tell(n, k):
        for steps in (n, N_Z - n):
            there = {"ep": lax.rem(ep + 2 * steps, N_EP), "tp": tp}
            pl.semaphore_signal(chain.at[k], inc=1, device_id=there, device_id_type=MESH)

    def told(k):
        with jax.named_scope("chain"):
            pl.semaphore_wait(chain.at[k], 2)

    tell(2, 0)
    sel_t = selb[...].astype(F32).T
    aff_t = affb[...].T
    lane2 = lax.broadcasted_iota(jnp.int32, (MOST, 2 * TOK), 1).astype(F32)
    lane1 = lax.broadcasted_iota(jnp.int32, (MOST, TOK), 1).astype(F32)
    for e in range(N_EP):
        column = sel_t[:, e : e + 1]
        spot = jnp.where(column < 0.0, float(TOK), column)
        onehot[e * MOST : (e + 1) * MOST] = jnp.where(lane2 == spot, 1.0, 0.0).astype(BF)
    sent[...] = (
        jnp.dot(onehot[...], tokb[...], preferred_element_type=F32).astype(BF).reshape(N_EP, MOST, WID)
    )

    def send_to(ds):
        for i in range(1, N_EP):
            if min(PLACES[i][0], N_Z - PLACES[i][0]) in ds:
                e, peer = ep_peer(i)
                remote(sent.at[e], came.at[PAD + i], z_send.at[0], z_recv.at[stage_of(i)], peer).start()

    send_to((0, 1, 2))
    told(0)
    tell(2, 1)
    tell(4, 2)
    send_to((3, 4))
    told(1)
    send_to((5, 6))
    told(2)
    send_to((7, 8))
    came[PAD] = sent[ep]
    if PAD:
        came[:PAD] = jnp.zeros((PAD, MOST, WID), BF)
    result[...] = jnp.zeros_like(result)

    for q in range(N_EP * MOST // TOK):
        tall = []
        for e in range(q * PER, (q + 1) * PER):
            tall.append(jnp.where(lane1 == sel_t[:, e : e + 1], aff_t[:, e : e + 1], 0.0))
        wide = jnp.concatenate(tall, axis=0).T
        high = wide.astype(BF)
        mix[:TOK, q * TOK : (q + 1) * TOK] = high
        mix[TOK:, q * TOK : (q + 1) * TOK] = (wide - high.astype(F32)).astype(BF)

    lane_row = lax.broadcasted_iota(jnp.int32, (1, WID), 1)
    lane_slot = lax.rem(lane_row, MOST).astype(F32)
    lane_group = lane_row // MOST

    starts, counts = [], []
    total = jnp.zeros((1, WID), F32)
    gathers = {}

    def wait_for(block, semaphore):
        pltpu.make_async_copy(block, block, semaphore).wait()

    def span(c, half):
        n = (EDGES[c + 1] - EDGES[c]) // 2
        return pl.ds(EDGES[c] + half * n, n)

    def first_half(c):
        return pl.ds(0, (EDGES[c + 1] - EDGES[c]) // 2)

    def begin_gather(c):
        for i in (2, 1, 3):
            for half in (0, 1):
                block = rows.at[tp, span(c, half)]
                copy = remote(
                    block, block, a1_send.at[0], a1_recv.at[c, half, i], line(half, i)[1]
                )
                copy.start()
                gathers[c, half, i] = copy
        for i in (2, 1, 3):
            for half in (0, 1):
                block = rows.at[tp, span(c, half)]
                remote(block, block, a2_send.at[0], a2_recv.at[c], line(1 - half, i)[1]).start()

    def pick_rows(c):
        nonlocal total
        low, high = EDGES[c], EDGES[c + 1]
        before, known = len(counts), known_at(c)
        with jax.named_scope("zwait"):
            new = max(before, 1)
            wait_for(came.at[pl.ds(PAD + new, known - new)], z_recv.at[c])
        for j in range(before, known):
            live = jnp.where(came[PAD + j].astype(F32) < DEAD / 2, 1.0, 0.0)
            n = jnp.sum(live, axis=0, keepdims=True)
            counts.append(n)
            starts.append(total)
            total = total + n
        down_rows = lax.broadcasted_iota(jnp.int32, (high - low, WID), 0).astype(F32) + float(low)
        none = jnp.zeros((1, WID), F32)
        for t in range(TILES):
            first, many = none, none
            for k in range(PER):
                j = known - TILES * PER + t * PER + k
                first = jnp.where(lane_group == k, starts[j] if j >= 0 else none, first)
                many = jnp.where(lane_group == k, counts[j] if j >= 0 else none, many)
            place = jnp.where(lane_slot < many, first + lane_slot, -1.0)
            pick[: high - low, t * WID : (t + 1) * WID] = jnp.where(down_rows == place, 1.0, 0.0).astype(BF)
        block = came[PAD + known - TILES * PER : PAD + known].reshape(TILES * WID, WID)
        rows[tp, low:high] = jnp.dot(pick[: high - low], block, preferred_element_type=F32).astype(BF)
        begin_gather(c)

    def pass_on(c):
        for j in (1, 3, 2):
            for half in (0, 1):
                with jax.named_scope("pass_wait"):
                    gathers[c, half, j].wait_recv()
                source = line(half, SIDE - j)[0]
                block = rows.at[source, span(c, half)]
                for i in (2, 1, 3):
                    remote(block, block, a2_send.at[0], a2_recv.at[c], line(1 - half, i)[1]).start()

    def place_rows(_):
        down_slots = lax.broadcasted_iota(jnp.int32, (MOST, WID), 0).astype(F32)
        lanes = lax.broadcasted_iota(jnp.int32, (MOST, WID), 1).astype(F32)
        for j in range(N_EP):
            place = jnp.where(down_slots < counts[j], starts[j] + down_slots, -1.0)
            for q in range(ROWS // WID):
                spread[j * MOST : (j + 1) * MOST, q * WID : (q + 1) * WID] = jnp.where(
                    lanes + float(q * WID) == place, 1.0, 0.0
                ).astype(BF)

    def compute(c):
        with jax.named_scope("gather_wait"):
            wait_for(rows.at[pl.ds(0, N_TP - SIDE), pl.ds(EDGES[c], EDGES[c + 1] - EDGES[c])], a2_recv.at[c])
        if c == 0:
            for load in loads[3:]:
                load.wait()
        at = slice(EDGES[c], EDGES[c + 1])
        chosen = jnp.concatenate([rows[k, at] for k in range(N_TP)], axis=1)
        both = jnp.dot(chosen, wgu[...], preferred_element_type=F32)
        gate, up = both[:, :WID], both[:, WID:]
        hidden = (gate / (1.0 + jnp.exp(-gate)) * up).astype(BF)
        partial = jnp.dot(hidden, wdb[...], preferred_element_type=F32).astype(BF)
        for k in range(N_TP):
            part[k // SIDE, k % SIDE, at] = partial[:, k * WID : (k + 1) * WID]

    def begin_sum(c):
        for i in (2, 1, 3):
            for half in (0, 1):
                t, peer = line(half, i)
                if half == 0:
                    block = part.at[:, t % SIDE, span(c, half)]
                else:
                    block = part.at[t // SIDE, :, span(c, half)]
                there = got1.at[c, half, i - 1, :, first_half(c)]
                remote(block, there, r1_send.at[0], r1_recv.at[c, half], peer).start()

    def go_on_sum(c):
        for half in (0, 1):
            with jax.named_scope("sum1_wait"):
                wait_for(got1.at[c, half, :, :, first_half(c)], r1_recv.at[c, half])
            mine = part[:, x, span(c, half)] if half == 0 else part[y, :, span(c, half)]
            added = mine.astype(F32)
            for i in range(3):
                added = added + got1[c, half, i, :, first_half(c)].astype(F32)
            sum1[c, half, :, first_half(c)] = added.astype(BF)
            for i in (2, 1, 3):
                t, peer = line(1 - half, i)
                block = sum1.at[c, half, t // SIDE if half == 0 else t % SIDE, first_half(c)]
                remote(block, got2.at[c, half, i - 1, first_half(c)], r2_send.at[0], r2_recv.at[c], peer).start()

    done, left = set(), list(range(N_EP))

    def give_back(js):
        first, last = js[0], js[-1] + 1
        low = EDGES[chunks_of(first)[0]] // WID * WID
        high = -(-EDGES[chunks_of(js[-1])[-1] + 1] // WID) * WID
        slots = jnp.dot(
            spread[first * MOST : last * MOST, low:high],
            result[low:high],
            preferred_element_type=F32,
        ).astype(BF)
        back[first:last] = slots.reshape(last - first, MOST, WID)
        for i in reversed(js):
            if i == 0:
                home[ep] = back[0]
            else:
                remote(back.at[i], home.at[ep], b_send.at[0], b_recv.at[0], ep_back(i)[1]).start()

    def end_sum(c):
        with jax.named_scope("sum2_wait"):
            wait_for(got2.at[c, :, :, first_half(c)], r2_recv.at[c])
        for half in (0, 1):
            added = sum1[c, half, y if half == 0 else x, first_half(c)].astype(F32)
            for i in range(3):
                added = added + got2[c, half, i, first_half(c)].astype(F32)
            result[span(c, half)] = added.astype(BF)
        done.add(c)
        ready = [i for i in left if done.issuperset(chunks_of(i))]
        runs = []
        for i in ready:
            left.remove(i)
            if runs and runs[-1][-1] == i - 1 and len(runs[-1]) < MOST // 4:
                runs[-1].append(i)
            else:
                runs.append([i])
        for js in reversed(runs):
            give_back(js)

    steps = {
        "Z": pick_rows,
        "F": pass_on,
        "P": place_rows,
        "K": compute,
        "B": begin_sum,
        "S": go_on_sum,
        "E": end_sum,
    }
    for step in STEPS:
        steps[step[0]](int(step[1:] or 0))

    wait_for(sent.at[pl.ds(1, N_EP - 1)], z_send.at[0])
    wait_for(rows.at[pl.ds(0, 3)], a1_send.at[0])
    wait_for(rows.at[pl.ds(0, 12)], a2_send.at[0])
    wait_for(rows.at[pl.ds(0, 12)], r1_send.at[0])
    wait_for(rows.at[pl.ds(0, 3)], r2_send.at[0])
    wait_for(back.at[pl.ds(1, N_EP - 1)], b_send.at[0])
    with jax.named_scope("home_wait"):
        wait_for(home.at[pl.ds(1, N_EP - 1)], b_recv.at[0])
    slots = home[...].reshape(N_EP * MOST, WID)
    weighted = jnp.dot(mix[...], slots, preferred_element_type=F32)
    out[...] = (weighted[:TOK] + weighted[TOK:]).astype(BF)


def per_device(tokens, selected, affinity, w_gate, w_up, w_down):
    width = tokens.shape[1]
    dma = pltpu.SemaphoreType.DMA
    scratch = [
        pltpu.VMEM((2 * TOK, WID), BF),
        pltpu.VMEM((N_EP, MOST), jnp.int32),
        pltpu.VMEM((N_EP, MOST), F32),
        pltpu.VMEM((width, 2 * WID), BF),
        pltpu.VMEM((WID, width), BF),
        pltpu.VMEM((N_EP * MOST, 2 * TOK), BF),
        pltpu.VMEM((N_EP, MOST, WID), BF),
        pltpu.VMEM((PAD + N_EP, MOST, WID), BF),
        pltpu.VMEM((LARGEST, TILES * WID), BF),
        pltpu.VMEM((N_EP * MOST, ROWS), BF),
        pltpu.VMEM((N_TP, ROWS, WID), BF),
        pltpu.VMEM((SIDE, SIDE, ROWS, WID), BF),
        pltpu.VMEM((CHUNKS, 2, 3, SIDE, LARGEST // 2, WID), BF),
        pltpu.VMEM((CHUNKS, 2, SIDE, LARGEST // 2, WID), BF),
        pltpu.VMEM((CHUNKS, 2, 3, LARGEST // 2, WID), BF),
        pltpu.VMEM((ROWS, WID), BF),
        pltpu.VMEM((N_EP, MOST, WID), BF),
        pltpu.VMEM((N_EP, MOST, WID), BF),
        pltpu.VMEM((2 * TOK, N_EP * MOST), BF),
        pltpu.SemaphoreType.REGULAR((3,)),
        dma((6,)),
        dma((1,)),
        dma((CHUNKS,)),
        dma((1,)),
        dma((CHUNKS, 2, 4)),
        dma((1,)),
        dma((CHUNKS,)),
        dma((1,)),
        dma((CHUNKS, 2)),
        dma((1,)),
        dma((CHUNKS,)),
        dma((1,)),
        dma((1,)),
    ]
    return pl.pallas_call(
        kernel,
        out_shape=jax.ShapeDtypeStruct((tokens.shape[0], WID), BF),
        in_specs=[pl.BlockSpec(memory_space=pl.ANY)] * 6,
        out_specs=pl.BlockSpec(memory_space=pltpu.VMEM),
        scratch_shapes=scratch,
        compiler_params=pltpu.CompilerParams(
            collective_id=0, has_side_effects=True, vmem_limit_bytes=67043328
        ),
    )(tokens, selected, affinity, w_gate[0], w_up[0], w_down[0])


def solution(mesh):
    return jax.shard_map(
        per_device,
        mesh=mesh,
        in_specs=(
            P("ep", None),
            P(None, "ep"),
            P(None, "ep"),
            P("ep", None, "tp"),
            P("ep", None, "tp"),
            P("ep", "tp", None),
        ),
        out_specs=P("ep", "tp"),
        check_vma=False,
    )
```
